32 devices in a mesh: fs: 8 (over z, y), tp: 4 (over x, core).
Axes of the slice: x: 2, y: 2, z: 4, core: 2. Of those that a mesh axis runs over, the one named last changes fastest.
Arguments:
- tokens: bfloat16 [6144, 2048], P('fs'), may hold values from -6 to 6
- norm_gain: float32 [2048], P('fs'), may hold values from 0.1 to 1.9
- gate_weight: float32 [2048, 5632], P('fs', 'tp'), may hold values from -0.125 to 0.125
- up_weight: float32 [2048, 5632], P('fs', 'tp'), may hold values from -0.125 to 0.125
- down_weight: float32 [5632, 2048], P('fs', 'tp'), may hold values from -0.078125 to 0.078125
Outputs:
- gate_out: bfloat16 [2048, 5632], P(None, 'tp')
- up_out: bfloat16 [2048, 5632], P(None, 'tp')
- down_out: bfloat16 [5632, 2048], P('tp')
- mixed: bfloat16 [6144, 2048], P('fs', 'tp')
The draws below stay inside these ranges and needn't reach their ends.
All inputs are finite; a program needn't handle non-finite values.
Results may differ from the reference program's by a relative error of at most 0.0095.
Values may be sent and summed in bfloat16 or wider, within the bound.
No kernel may reach another device: no remote copies, remote signals or barrier semaphores. Data moves between devices by JAX's collectives and lax.ppermute only.
A program may use at most 128 MiB of HBM per device.

```python
import jax
import jax.numpy as jnp
from jax import lax

D = 2048
FF = 5632
TOKENS = 6144
N_TP = 4


def level_of(stream_key, dims, cuts, least, largest):
    gain, own = 1.0, jax.random.fold_in(stream_key, 6)
    for dim, blocks in cuts:
        heights = jnp.exp(jax.random.uniform(jax.random.fold_in(own, dim), (blocks,), jnp.float32, least / len(cuts), largest / len(cuts)))
        gain = gain * jnp.repeat(heights, dims[dim] // blocks).reshape([-1 if axis == dim else 1 for axis in range(len(dims))])
    return gain


def centred(rng, dims, width, reach, cuts=(), kind=jnp.bfloat16):
    result = width * jax.random.normal(rng, dims, jnp.float32)
    if cuts:
        result = result * level_of(rng, dims, cuts, -0.22, 0.18)
    return jnp.clip(result, -reach, reach).astype(kind)


def setup_inputs(seed: int = 0) -> dict:
    splits = jax.random.split(jax.random.key(seed), 6)
    return {
        "tokens": centred(splits[0], (TOKENS, D), 1.0, 6.0, ((0, 8),)),
        "norm_gain": jnp.clip(1.0 + 0.18 * jax.random.normal(splits[1], (D,), jnp.float32), 0.1, 1.9),
        "gate_weight": centred(splits[2], (D, FF), D ** -0.5, 0.125, ((0, 8), (1, 4)), jnp.float32),
        "up_weight": centred(splits[3], (D, FF), D ** -0.5, 0.125, ((0, 8), (1, 4)), jnp.float32),
        "down_weight": centred(splits[4], (FF, D), FF ** -0.5, 0.078125, ((0, 8), (1, 4)), jnp.float32),
    }


eps_norm = 1e-06

def reference(tokens, norm_gain, gate_weight, up_weight, down_weight):
    gain_column = norm_gain[:, None]
    gate_out = (gate_weight * gain_column).astype(jnp.bfloat16)
    up_out = (up_weight * gain_column).astype(jnp.bfloat16)
    down_out = down_weight.astype(jnp.bfloat16)
    rows_float = tokens.astype(jnp.float32)
    normed = (rows_float * lax.rsqrt(lax.optimization_barrier(jnp.mean(rows_float * rows_float, axis=-1, keepdims=True)) + eps_norm)).astype(jnp.bfloat16)
    gate_act = jnp.dot(normed, gate_out, preferred_element_type=jnp.float32)
    up_act = jnp.dot(normed, up_out, preferred_element_type=jnp.float32)
    hidden = (jax.nn.silu(gate_act) * up_act).astype(jnp.bfloat16)
    block_rows = FF // N_TP
    total = jnp.zeros((tokens.shape[0], D), jnp.float32)
    for index in range(N_TP):
        lower = index * block_rows
        share = jnp.dot(hidden[:, lower:lower + block_rows], down_out[lower:lower + block_rows, :], preferred_element_type=jnp.float32).astype(jnp.bfloat16)
        total = total + share.astype(jnp.float32)
    mixed = total.astype(jnp.bfloat16)
    return (gate_out, up_out, down_out, mixed)
```

```python
import jax
import jax.numpy as jnp
from jax import lax
from jax.sharding import PartitionSpec as P

eps_norm = 1e-06


def ring_order(n):
    if n % 2:
        return list(range(n))
    return list(range(0, n, 2)) + list(range(n - 1, 0, -2))


def piece_widths(total):
    lanes = total // 128
    count = min(4, lanes)
    sizes = [lanes // count + (1 if i < lanes % count else 0) for i in range(count)]
    widths = [s * 128 for s in sizes]
    widths[-1] += total - sum(widths)
    return widths


def after(value, dep):
    if dep is None:
        return value
    return lax.optimization_barrier((value, dep))[0]


class Line:
    def __init__(self, perm, window):
        self.perm, self.window, self.done = perm, window, []

    def send(self, value):
        if len(self.done) >= self.window:
            value = after(value, self.done[-self.window])
        got = lax.ppermute(value, "fs", self.perm)
        self.done.append(got)
        return got


def make_on_device(n_fs, n_tp):
    order = ring_order(n_fs)
    fwd = [(order[i], order[(i + 1) % n_fs]) for i in range(n_fs)]
    bwd = [(b, a) for a, b in fwd]
    half = n_fs // 2

    def source_of(ring_pos):
        p = lax.rem(ring_pos + 2 * n_fs, n_fs)
        if n_fs % 2:
            return p
        return jnp.where(p < half, 2 * p, 2 * (n_fs - 1 - p) + 1)

    def on_device(tokens, norm_gain, gate_weight, up_weight, down_weight):
        f = lax.axis_index("fs")
        t = lax.axis_index("tp")
        pos = f if n_fs % 2 else jnp.where(f % 2 == 0, f // 2, n_fs - 1 - f // 2)
        rows = gate_weight.shape[0]
        ff = gate_weight.shape[1]
        d_rows, d_cols = down_weight.shape
        lines = (Line(fwd, 2), Line(bwd, 2))

        def gather(arrays):
            results = [[(a, f)] for a in arrays]
            state = [[a, a] for a in arrays]
            longer = [i % 2 for i in range(len(arrays))]
            long_hops, short_hops = n_fs // 2, n_fs - 1 - n_fs // 2
            for step in range(1, long_hops + 1):
                for i in range(len(arrays)):
                    for side in (0, 1):
                        hops = long_hops if side == longer[i] else short_hops
                        if step <= hops:
                            got = lines[side].send(state[i][side])
                            state[i][side] = got
                            src = source_of(pos - step if side == 0 else pos + step)
                            results[i].append((got, src))
            return results

        down_cast = down_weight.astype(jnp.bfloat16)
        top = d_rows // 2
        parts = gather([down_cast[:top], down_cast[top:]])
        column_block = jnp.zeros((n_fs * d_rows, d_cols), jnp.bfloat16)
        for offset, part in zip((0, top), parts):
            for chunk, src in part:
                column_block = lax.dynamic_update_slice(column_block, chunk, (src * d_rows + offset, 0))

        block_rows = n_fs * d_rows // n_tp
        down_out = jnp.zeros((block_rows, n_tp * d_cols), jnp.bfloat16)
        for d in range(n_tp):
            to = lax.bitwise_xor(t, d)
            block = lax.dynamic_slice(column_block, (to * block_rows, 0), (block_rows, d_cols))
            if d:
                block = lax.ppermute(block, "tp", [(i, i ^ d) for i in range(n_tp)])
            down_out = lax.dynamic_update_slice(down_out, block, (0, to * d_cols))

        rows_float = tokens.astype(jnp.float32)
        normed = (
            rows_float * lax.rsqrt(jnp.mean(rows_float * rows_float, axis=-1, keepdims=True) + eps_norm)
        ).astype(jnp.bfloat16)
        normed = lax.optimization_barrier(normed)

        gain_column = norm_gain[:, None]
        widths = piece_widths(ff)
        offsets = [sum(widths[:i]) for i in range(len(widths))]
        messages = [
            jnp.concatenate(
                [
                    (gate_weight[:, o : o + w] * gain_column).astype(jnp.bfloat16),
                    (up_weight[:, o : o + w] * gain_column).astype(jnp.bfloat16),
                ],
                axis=1,
            )
            for o, w in zip(offsets, widths)
        ]
        gate_out = jnp.zeros((n_fs * rows, ff), jnp.bfloat16)
        up_out = jnp.zeros((n_fs * rows, ff), jnp.bfloat16)
        mixed = None
        for first in range(0, len(widths), 2):
            group = list(range(first, min(first + 2, len(widths))))
            gathered = gather([messages[i] for i in group])
            for i, part in zip(group, gathered):
                o, w = offsets[i], widths[i]
                whole = jnp.zeros((n_fs * rows, 2 * w), jnp.bfloat16)
                for chunk, src in part:
                    whole = lax.dynamic_update_slice(whole, chunk, (src * rows, 0))
                gate_out = lax.dynamic_update_slice(gate_out, whole[:, :w], (0, o))
                up_out = lax.dynamic_update_slice(up_out, whole[:, w:], (0, o))
                act = jnp.dot(normed, whole, preferred_element_type=jnp.float32)
                hidden = (jax.nn.silu(act[:, :w]) * act[:, w:]).astype(jnp.bfloat16)
                have = [(0, hidden)]
                bit = n_tp // 2
                while bit:
                    have = have + [
                        (d ^ bit, lax.ppermute(h, "tp", [(k, k ^ bit) for k in range(n_tp)])) for d, h in have
                    ]
                    bit //= 2
                for d, h in have:
                    start = lax.bitwise_xor(t, d) * block_rows + o
                    down_part = lax.dynamic_slice(column_block, (start, 0), (w, d_cols))
                    term = jnp.dot(h, down_part, preferred_element_type=jnp.float32)
                    mixed = term if mixed is None else mixed + term
        return gate_out, up_out, down_out, mixed.astype(jnp.bfloat16)

    return on_device


def solution(mesh):
    in_specs = (P("fs", None), P("fs"), P("fs", "tp"), P("fs", "tp"), P("fs", "tp"))
    out_specs = (P(None, "tp"), P(None, "tp"), P("tp", None), P("fs", "tp"))
    return jax.shard_map(
        make_on_device(mesh.shape["fs"], mesh.shape["tp"]),
        mesh=mesh,
        in_specs=in_specs,
        out_specs=out_specs,
        check_vma=False,
    )
```
